32 devices in a mesh: sp: 16 (over z, y, x), tp: 2 (over core).
Axes of the slice: x: 2, y: 2, z: 4, core: 2. Of those that a mesh axis runs over, the one named last changes fastest.
Arguments:
- tokens: bfloat16 [8192, 2048], P('sp', 'tp'), may hold values from -6 to 6
- input_gain: bfloat16 [2048], P('tp'), may hold values from 0.099609375 to 1.8984375
- query_weight: bfloat16 [2048, 1024], P(None, 'tp'), may hold values from -10 to 10
- key_weight: bfloat16 [2048, 1024], P(None, 'tp'), may hold values from -10 to 10
- value_weight: bfloat16 [2048, 1024], P(None, 'tp'), may hold values from -0.125 to 0.125
- pool_in_weight: bfloat16 [2048, 1024], P(None, 'tp'), may hold values from -0.125 to 0.125
- log_gates: float32 [8, 8192], P('tp'), may hold values from -8192 to 0, as said below
- pool_weight: bfloat16 [8, 128, 128], P('tp'), may hold values from -0.5 to 0.5
- pool_scale: float32 [1024], P('tp'), may hold values from 0.1 to 1.9
- attention_out: bfloat16 [1024, 2048], P('tp'), may hold values from -16 to 16
- pooling_out: bfloat16 [1024, 2048], P('tp'), may hold values from -16 to 16
- final_gain: float32 [2048], P('tp'), may hold values from 0.1 to 1.9
Outputs:
- layer_out: bfloat16 [8192, 2048], P('sp', 'tp')
The draws below stay inside these ranges and needn't reach their ends.
Inputs may be any that keep to these rules, and one draw needn't show every extreme that they name: `log_gates`: each row does not increase along positions.
All inputs are finite; a program needn't handle non-finite values.
Results may differ from the reference program's by a relative error of at most 0.015.
Values may be sent and summed in bfloat16 or wider, within the bound.
A program may use at most 128 MiB of HBM per device.

```python
import math
import jax
import jax.numpy as jnp
from jax import lax

D = 2048
HEAD = 128
ATT_HEADS = 8
POOL_GROUPS = 8
TOK_DEV = 512
TOKENS = 8192


def pair_bases(key):
    first = jnp.clip(jax.random.normal(jax.random.fold_in(key, 101), (D, ATT_HEADS * HEAD), jnp.float32), -4.0, 4.0)
    second = jnp.clip(jax.random.normal(jax.random.fold_in(key, 102), (D, ATT_HEADS * HEAD), jnp.float32), -4.0, 4.0)
    return (first, second)


def draw_query_weight(key, part):
    first, second = pair_bases(key)
    drawn = first
    return (drawn * D ** (-0.5)).astype(jnp.bfloat16)


def draw_key_weight(key, part):
    first, second = pair_bases(key)
    drawn = 3.0 * second
    return (drawn * D ** (-0.5)).astype(jnp.bfloat16)


def draw_log_gates(key, part):
    heads = ATT_HEADS
    order = jax.random.permutation(jax.random.fold_in(key, 31), heads)
    slow = order < heads // 2
    forget_span = jnp.exp(jax.random.uniform(jax.random.fold_in(key, 32), (heads,), jnp.float32, math.log(30.0), math.log(100.0)))
    starting_shift_amount = jnp.where(slow, 0.55 / TOKENS, 1.0 / forget_span)
    approximate_guess = jnp.exp(jax.random.uniform(jax.random.fold_in(key, 33), (heads, TOKENS), jnp.float32, -math.log(4.0), math.log(4.0)))
    blocks = jnp.exp(jax.random.uniform(jax.random.fold_in(key, 34), (heads, TOKENS // TOK_DEV), jnp.float32, -math.log(2.0), math.log(2.0)))
    tile_scaling_factor = jnp.repeat(blocks, TOK_DEV, axis=1)
    seat_indices = jax.random.randint(jax.random.fold_in(key, 35), (heads, 2), 0, TOKENS)
    objective_numbers = jnp.log(jax.random.uniform(jax.random.fold_in(key, 36), (heads, 2), jnp.float32, 0.5, 0.8))
    element_locations = jnp.arange(TOKENS, dtype=jnp.int32)
    segment_clusters = jnp.sum(jnp.where(element_locations[None, None, :] == seat_indices[:, :, None], objective_numbers[:, :, None], 0.0), axis=1)
    return jnp.cumsum(segment_clusters - starting_shift_amount[:, None] * approximate_guess * tile_scaling_factor, axis=1).astype(jnp.float32)


def rising_weight(key, rows, salt):
    noise = jnp.clip(jax.random.normal(jax.random.fold_in(key, salt), (rows, D), jnp.float32), -4.0, 4.0)
    highest = 10.0
    jitter = jnp.exp(jax.random.uniform(jax.random.fold_in(key, salt + 1), (D,), jnp.float32, -0.35, 0.35))
    rising = jnp.exp(math.log(highest) * jnp.arange(D, dtype=jnp.float32) / D) * jitter
    return (noise * rising[None, :] * rows ** (-0.5)).astype(jnp.bfloat16)


def draw_attention_out(key, part):
    return rising_weight(key, ATT_HEADS * HEAD, 41)


def draw_pooling_out(key, part):
    return rising_weight(key, POOL_GROUPS * HEAD, 51)


def levels(rng, dims, shards, low, largest):
    def one(dim, blocks):
        heights = jax.random.uniform(jax.random.fold_in(jax.random.fold_in(rng, 6), dim), (blocks,), jnp.float32, low / len(shards), largest / len(shards))
        return jnp.repeat(jnp.exp(heights), dims[dim] // blocks).reshape((-1,) + (1,) * (len(dims) - dim - 1))

    gain = one(*shards[0])
    for cut in shards[1:]:
        gain = gain * one(*cut)
    return gain


def bell_draw(stream_key, shape, scale, bound, split=(), kind=jnp.bfloat16):
    level = levels(stream_key, shape, split, -0.22, 0.18) if split else 1.0
    values = jax.random.normal(stream_key, shape, jnp.float32) * scale * level
    return jnp.minimum(jnp.maximum(values, -bound), bound).astype(kind)


def setup_inputs(seed: int = 0) -> dict:
    splits = jax.random.split(jax.random.key(seed), 13)
    tokens = bell_draw(splits[0], (TOKENS, D), 1.0, 6.0, ((0, 16), (1, 2)))
    input_gain = jnp.clip(1.0 + 0.18 * jax.random.normal(splits[1], (D,), jnp.float32), 0.099609375, 1.8984375).astype(jnp.bfloat16)
    query_weight = draw_query_weight(jax.random.fold_in(splits[12], 71), 0)
    key_weight = draw_key_weight(jax.random.fold_in(splits[12], 71), 0)
    value_weight = bell_draw(splits[4], (D, ATT_HEADS * HEAD), D ** -0.5, 0.125, ((1, 2),))
    pool_in_weight = bell_draw(splits[5], (D, POOL_GROUPS * HEAD), D ** -0.5, 0.125, ((1, 2),))
    log_gates = draw_log_gates(jax.random.fold_in(splits[12], 71), 0)
    pool_weight = bell_draw(splits[7], (POOL_GROUPS, HEAD, HEAD), HEAD ** -0.5, 0.5, ((0, 2),))
    pool_scale = jnp.clip(1.0 + 0.18 * jax.random.normal(splits[8], (POOL_GROUPS * HEAD,), jnp.float32), 0.1, 1.9)
    attention_out = draw_attention_out(jax.random.fold_in(splits[12], 71), 0)
    pooling_out = draw_pooling_out(jax.random.fold_in(splits[12], 71), 0)
    final_gain = jnp.clip(1.0 + 0.18 * jax.random.normal(splits[11], (D,), jnp.float32), 0.1, 1.9)
    return {"tokens": tokens, "input_gain": input_gain, "query_weight": query_weight, "key_weight": key_weight, "value_weight": value_weight, "pool_in_weight": pool_in_weight, "log_gates": log_gates, "pool_weight": pool_weight, "pool_scale": pool_scale, "attention_out": attention_out, "pooling_out": pooling_out, "final_gain": final_gain}


epsilon = 1e-06

def attention(query, keys, values, log_gates):
    total_rows = query.shape[0]
    heads = log_gates.shape[0]
    head_size = query.shape[1] // heads
    block = math.gcd(total_rows, 256)
    query_blocks = query.reshape(total_rows // block, block, heads, head_size).astype(jnp.float32)
    keys_whole = keys.reshape(total_rows, heads, head_size).astype(jnp.float32)
    values_whole = values.reshape(total_rows, heads, head_size).astype(jnp.float32)
    key_rows = jnp.arange(total_rows, dtype=jnp.int32)

    def one_block(args):
        query_block, first = args
        query_gate = lax.dynamic_slice_in_dim(log_gates, first, block, 1).T
        scores = jnp.einsum('thd,shd->ths', query_block, keys_whole) * head_size ** (-0.5)
        scores = scores + query_gate[:, :, None] - log_gates[None, :, :]
        rows = first + jnp.arange(block, dtype=jnp.int32)
        allowed = (rows[:, None] >= key_rows[None, :])[:, None, :]
        scores = jnp.where(allowed, scores, -jnp.inf)
        row_max = lax.optimization_barrier(jnp.max(scores, axis=2, keepdims=True))
        weights = jnp.exp(scores - row_max)
        totals = lax.optimization_barrier(jnp.sum(weights, axis=2))
        rounded = lax.optimization_barrier(weights.astype(jnp.bfloat16)).astype(jnp.float32)
        result = jnp.einsum('ths,shd->thd', rounded, values_whole) / totals[:, :, None]
        return result.astype(jnp.bfloat16)
    block_starts = jnp.arange(total_rows // block, dtype=jnp.int32) * block
    result = lax.map(one_block, (query_blocks, block_starts))
    return result.reshape(total_rows, heads * head_size)

def pooling(pool_input, pool_weight, pool_scale):
    total_rows, width = pool_input.shape
    groups = pool_weight.shape[0]
    head_size = pool_weight.shape[1]
    widened = pool_input.astype(jnp.float32)
    running = jnp.cumsum(widened, axis=0)
    padded = jnp.concatenate([jnp.zeros((1, width), jnp.float32), running], axis=0)
    rows = jnp.arange(total_rows, dtype=jnp.int32)[:, None]
    column = jnp.arange(width, dtype=jnp.int32)
    window = jnp.left_shift(jnp.full((width,), 2, jnp.int32), column // head_size % 4)
    lower = jnp.maximum(rows + 1 - window[None, :], 0).astype(jnp.int32)
    counts = (rows + 1 - lower).astype(jnp.float32)
    window_sum = running - jnp.take_along_axis(padded, lower, axis=0)
    departure = (window_sum / counts - widened).astype(jnp.bfloat16)
    mapped = jnp.einsum('tgc,gcd->tgd', departure.reshape(total_rows, groups, head_size).astype(jnp.float32), pool_weight.astype(jnp.float32))
    return (mapped.reshape(total_rows, width) * pool_scale).astype(jnp.bfloat16)

def reference(tokens, input_gain, query_weight, key_weight, value_weight, pool_in_weight, log_gates, pool_weight, pool_scale, attention_out, pooling_out, final_gain):
    widened = tokens.astype(jnp.float32)
    inverse = lax.rsqrt(lax.optimization_barrier(jnp.mean(widened * widened, axis=1)) + epsilon)[:, None]
    scaled = (widened * input_gain.astype(jnp.float32)).astype(jnp.bfloat16)

    def project(weight):
        return (jnp.dot(scaled, weight, preferred_element_type=jnp.float32) * inverse).astype(jnp.bfloat16)
    attended = attention(project(query_weight), project(key_weight), project(value_weight), log_gates)
    pooled = pooling(project(pool_in_weight), pool_weight, pool_scale)
    mixed = jnp.dot(attended, attention_out, preferred_element_type=jnp.float32) + jnp.dot(pooled, pooling_out, preferred_element_type=jnp.float32)
    out_inverse = lax.rsqrt(lax.optimization_barrier(jnp.mean(mixed * mixed, axis=1)) + epsilon)[:, None]
    return (mixed * out_inverse * final_gain).astype(jnp.bfloat16)
```

```python
import functools

import jax
import jax.numpy as jnp
from jax import lax
from jax.experimental import pallas as pl
from jax.experimental.pallas import tpu as pltpu
from jax.sharding import PartitionSpec as P

WINDOW_MAX = 16
LANES = 128
LOG2E = 1.4426950408889634

very_low = -1e30
epsilon = 1e-06


def passed_along(block, axis, distance):
    devices = range(lax.axis_size(axis))
    route = [(i - distance, i) for i in devices if i - distance in devices]
    return lax.ppermute(block, axis, route)


def swapped(block, axis, offset):
    return lax.ppermute(block, axis, [(i, i ^ offset) for i in range(lax.axis_size(axis))])


def attend_kernel(first, last, heads, head_size, chunk, mode_ref, start_ref, *refs):
    if first:
        q_ref, kv_ref, gate_ref, acc_out, ml_out = refs
    else:
        q_ref, kv_ref, gate_ref, acc_in, ml_in, acc_out, ml_out = refs
    slot = pl.program_id(0)
    rows = q_ref.shape[1]
    keys = kv_ref.shape[0]
    width = heads * head_size
    lane = lax.broadcasted_iota(jnp.int32, (chunk, LANES), 1)

    def state_of(r, h):
        if first:
            return None
        ml = ml_in[0, r : r + chunk, :]
        columns = slice(h * head_size, (h + 1) * head_size)
        return (ml[:, h : h + 1], ml[:, heads + h : heads + h + 1], acc_in[0, r : r + chunk, columns])

    def store(r, h, ml, state):
        columns = slice(h * head_size, (h + 1) * head_size)
        high, total, summed = state
        if last:
            safe = jnp.where(total > 0.0, total, 1.0)
            acc_out[0, r : r + chunk, columns] = (summed / safe).astype(acc_out.dtype)
            level = jnp.where(total > 0.0, high + jnp.log2(safe), very_low)
            return jnp.where(lane == h, level, ml)
        acc_out[0, r : r + chunk, columns] = summed
        return jnp.where(lane == h, high, jnp.where(lane == heads + h, total, ml))

    def compute(diagonal):
        for r in range(0, rows, chunk):
            ml = jnp.zeros((chunk, LANES), jnp.float32)
            span = min(r + chunk, keys) if diagonal else keys
            for h in range(heads):
                columns = slice(h * head_size, (h + 1) * head_size)
                q = q_ref[0, r : r + chunk, columns]
                k = kv_ref[:span, columns]
                v = kv_ref[:span, width + h * head_size : width + (h + 1) * head_size]
                bias = (start_ref[slot * heads + h] - gate_ref[h : h + 1, :span]) * LOG2E
                s = lax.dot_general(q, k, (((1,), (1,)), ((), ())), preferred_element_type=jnp.float32)
                s = s + bias
                if diagonal:
                    row = r + lax.broadcasted_iota(jnp.int32, s.shape, 0)
                    s = jnp.where(row >= lax.broadcasted_iota(jnp.int32, s.shape, 1), s, very_low)
                old = state_of(r, h)
                high = jnp.max(s, axis=1, keepdims=True)
                if old is not None:
                    high = jnp.maximum(high, old[0])
                p = jnp.exp2(s - high)
                total = jnp.sum(p, axis=1, keepdims=True)
                summed = jnp.dot(p.astype(jnp.bfloat16), v, preferred_element_type=jnp.float32)
                if old is not None:
                    factor = jnp.exp2(old[0] - high)
                    total = total + factor * old[1]
                    summed = summed + factor * old[2]
                ml = store(r, h, ml, (high, total, summed))
            ml_out[0, r : r + chunk, :] = ml

    if first:
        pl.when(slot == 0)(lambda: compute(True))

        @pl.when((slot > 0) & (mode_ref[slot] > 0))
        def _():
            compute(False)

    else:

        @pl.when(mode_ref[slot] > 0)
        def _():
            compute(False)

    @pl.when((mode_ref[slot] == 0) & ((slot > 0) | (not first)))
    def _():
        for r in range(0, rows, chunk):
            ml = jnp.zeros((chunk, LANES), jnp.float32)
            for h in range(heads):
                old = state_of(r, h)
                if old is None:
                    old = (
                        jnp.full((chunk, 1), very_low, jnp.float32),
                        jnp.zeros((chunk, 1), jnp.float32),
                        jnp.zeros((chunk, head_size), jnp.float32),
                    )
                ml = store(r, h, ml, old)
            ml_out[0, r : r + chunk, :] = ml


def attend_step(mode, starts, queries, pair, gates, state, last, head_size):
    slots, rows, width = queries.shape
    heads = width // head_size
    first = state is None
    chunk = min(rows, 256)
    by_slot = lambda g, *_: (g, 0, 0)
    whole = lambda g, *_: (0, 0)
    in_specs = [
        pl.BlockSpec((1, rows, width), by_slot),
        pl.BlockSpec(pair.shape, whole),
        pl.BlockSpec(gates.shape, whole),
    ]
    state_specs = [pl.BlockSpec((1, rows, width), by_slot), pl.BlockSpec((1, rows, LANES), by_slot)]
    if not first:
        in_specs = in_specs + state_specs
    keys = pair.shape[0]
    return pl.pallas_call(
        functools.partial(attend_kernel, first, last, heads, head_size, chunk),
        out_shape=(
            jax.ShapeDtypeStruct((slots, rows, width), jnp.bfloat16 if last else jnp.float32),
            jax.ShapeDtypeStruct((slots, rows, LANES), jnp.float32),
        ),
        grid_spec=pltpu.PrefetchScalarGridSpec(
            num_scalar_prefetch=2, grid=(slots,), in_specs=in_specs, out_specs=state_specs
        ),
        compiler_params=pltpu.CompilerParams(dimension_semantics=("arbitrary",)),
        cost_estimate=pl.CostEstimate(
            flops=8 * slots * rows * keys * width,
            bytes_accessed=12 * slots * rows * width,
            transcendentals=slots * rows * keys * heads,
        ),
    )(mode, starts, queries, pair, gates, *(() if first else state))


def gathered(block, axis):
    if lax.axis_size(axis) != 2:
        return lax.all_gather(block, axis, axis=1, tiled=True)
    other = swapped(block, axis, 1)
    lower = lax.axis_index(axis) == 0
    return jnp.concatenate([jnp.where(lower, block, other), jnp.where(lower, other, block)], axis=1)


def body(
    tokens,
    input_gain,
    query_weight,
    key_weight,
    value_weight,
    pool_in_weight,
    log_gates,
    pool_weight,
    pool_scale,
    attention_out,
    pooling_out,
    final_gain,
):
    tok_rows = tokens.shape[0]
    width = query_weight.shape[0]
    groups = pool_weight.shape[0]
    head_size = pool_weight.shape[1]
    heads = log_gates.shape[0]
    attention_width = query_weight.shape[1]
    pool_width = pool_in_weight.shape[1]
    devices = lax.axis_size("sp")
    shards = lax.axis_size("tp")
    side = 1
    while (2 * side) ** 2 <= devices and devices % (2 * side) == 0:
        side = 2 * side
    planes = devices // side
    sequence_index = lax.axis_index("sp")
    plane = sequence_index // side
    seat = sequence_index % side
    first_row = sequence_index * tok_rows

    part = gathered(tokens, "tp")
    gain_part = gathered(input_gain.reshape(1, -1), "tp")
    widened = part.astype(jnp.float32)
    scaled = (widened * gain_part.astype(jnp.float32)).astype(jnp.bfloat16)

    def product(weight):
        return jnp.dot(scaled, weight, preferred_element_type=jnp.float32)

    inverse = lax.rsqrt(jnp.sum(widened * widened, axis=1) / width + epsilon)[:, None]
    keys = (product(key_weight) * inverse).astype(jnp.bfloat16)
    values = (product(value_weight) * inverse).astype(jnp.bfloat16)
    pair = jnp.concatenate([keys, values], axis=1)
    pairs = [pair]
    for k in range(1, planes):
        pairs.append(passed_along(pairs[-1], "sp", side))
    query = (product(query_weight) * (inverse * (LOG2E * head_size ** (-0.5)))).astype(jnp.bfloat16)
    queries = jnp.stack([query] + [swapped(query, "sp", g) for g in range(1, side)])

    pool_input = (product(pool_in_weight) * inverse).astype(jnp.bfloat16)
    rim = passed_along(pool_input[tok_rows - (WINDOW_MAX - 1) :], "sp", 1)

    seats = seat ^ jnp.arange(side, dtype=jnp.int32)
    starts = jnp.stack(
        [
            lax.dynamic_slice_in_dim(log_gates, (plane * side + (seat ^ g)) * tok_rows, 1, 1)[:, 0]
            for g in range(side)
        ]
    ).reshape(-1)
    state = None
    for k in range(planes):
        source = jnp.maximum(sequence_index - k * side, seat)
        gates = lax.dynamic_slice_in_dim(log_gates, source * tok_rows, tok_rows, 1)
        if k == 0:
            mode = (seats > seat).astype(jnp.int32)
        else:
            mode = jnp.full((side,), plane >= k, jnp.int32)
        state = attend_step(mode, starts, queries, pairs[k], gates, state, k == planes - 1, head_size)
    partial, level = state
    level = level[:, :, :heads]
    shares = [partial[0]] + [swapped(partial[g], "sp", g) for g in range(1, side)]
    tall = jnp.transpose(level, (0, 2, 1))
    levels = jnp.stack([tall[0]] + [swapped(tall[g], "sp", g) for g in range(1, side)])
    portion = jnp.exp2(levels - jnp.max(levels, axis=0, keepdims=True))
    portion = portion / jnp.sum(portion, axis=0, keepdims=True)
    portion = jnp.transpose(portion, (0, 2, 1))
    attended = 0.0
    for g in range(side):
        attended = attended + shares[g].astype(jnp.float32) * jnp.repeat(portion[g], head_size, axis=1)
    attended = attended.astype(jnp.bfloat16)

    extended = jnp.concatenate([rim, pool_input], axis=0).astype(jnp.float32)
    column = jnp.arange(pool_width, dtype=jnp.int32)
    group_number = lax.axis_index("tp") * groups + column // head_size
    window = jnp.left_shift(jnp.full((pool_width,), 2, jnp.int32), group_number % 4)
    sums = extended
    span = 1
    chosen = jnp.zeros((tok_rows, pool_width), jnp.float32)
    for level_number in range(4):
        sums = sums[span:] + sums[:-span]
        span = span * 2
        offset_rows = WINDOW_MAX - span
        chosen = jnp.where(window[None, :] == span, sums[offset_rows : offset_rows + tok_rows], chosen)
    element_locations = first_row + jnp.arange(tok_rows, dtype=jnp.int32)
    counts = jnp.minimum(window[None, :], element_locations[:, None] + 1).astype(jnp.float32)
    departure = (chosen / counts - pool_input.astype(jnp.float32)).astype(jnp.bfloat16)
    mapped = jnp.concatenate(
        [
            jnp.dot(
                departure[:, g * head_size : (g + 1) * head_size],
                pool_weight[g],
                preferred_element_type=jnp.float32,
            )
            for g in range(groups)
        ],
        axis=1,
    )
    pooled = (mapped * pool_scale).astype(jnp.bfloat16)
    pooled_part = jnp.dot(pooled, pooling_out, preferred_element_type=jnp.float32)
    whole = jnp.dot(attended, attention_out, preferred_element_type=jnp.float32) + pooled_part
    if shards == 2:
        half = width // 2
        lower = lax.axis_index("tp") == 0
        sent = jnp.where(lower, whole[:, half:], whole[:, :half]).astype(jnp.bfloat16)
        kept = jnp.where(lower, whole[:, :half], whole[:, half:])
        mixed = kept + swapped(sent, "tp", 1).astype(jnp.float32)
        squares = jnp.sum(mixed * mixed, axis=1)
        squares = squares + swapped(squares, "tp", 1)
    else:
        mixed = lax.psum_scatter(
            whole.astype(jnp.bfloat16), "tp", scatter_dimension=1, tiled=True
        ).astype(jnp.float32)
        squares = lax.psum(jnp.sum(mixed * mixed, axis=1), "tp")
    out_inverse = lax.rsqrt(squares / width + epsilon)
    return (mixed * out_inverse[:, None] * final_gain[None, :]).astype(jnp.bfloat16)


def solution(mesh):
    return jax.shard_map(
        body,
        mesh=mesh,
        in_specs=(
            P("sp", "tp"),
            P("tp"),
            P(None, "tp"),
            P(None, "tp"),
            P(None, "tp"),
            P(None, "tp"),
            P("tp", None),
            P("tp", None, None),
            P("tp"),
            P("tp", None),
            P("tp", None),
            P("tp"),
        ),
        out_specs=P("sp", "tp"),
        check_vma=False,
    )
```

```python
import functools

import jax
import jax.numpy as jnp
from jax import lax
from jax.experimental import pallas as pl
from jax.experimental.pallas import tpu as pltpu
from jax.sharding import PartitionSpec as P


WINDOW_MAX = 16
LANES = 128
LOG2E = 1.4426950408889634

very_low = -1e30
epsilon = 1e-06


def passed_along(block, axis, distance):
    devices = range(lax.axis_size(axis))
    route = [(i - distance, i) for i in devices if i - distance in devices]
    return lax.ppermute(block, axis, route)


def swapped(block, axis, offset):
    return lax.ppermute(block, axis, [(i, i ^ offset) for i in range(lax.axis_size(axis))])


def attend_kernel(first, last, heads, head_size, chunk, mode_ref, start_ref, *refs):
    if first:
        q_ref, kv_ref, gate_ref, acc_out, ml_out = refs
    else:
        q_ref, kv_ref, gate_ref, acc_in, ml_in, acc_out, ml_out = refs
    slot = pl.program_id(0)
    rows = q_ref.shape[1]
    keys = kv_ref.shape[0]
    width = heads * head_size
    lane = lax.broadcasted_iota(jnp.int32, (chunk, LANES), 1)

    def state_of(r, h):
        if first:
            return None
        ml = ml_in[0, r : r + chunk, :]
        columns = slice(h * head_size, (h + 1) * head_size)
        return (ml[:, h : h + 1], ml[:, heads + h : heads + h + 1], acc_in[0, r : r + chunk, columns])

    def store(r, h, ml, state):
        columns = slice(h * head_size, (h + 1) * head_size)
        high, total, summed = state
        if last:
            safe = jnp.where(total > 0.0, total, 1.0)
            acc_out[0, r : r + chunk, columns] = (summed / safe).astype(acc_out.dtype)
            level = jnp.where(total > 0.0, high + jnp.log2(safe), very_low)
            return jnp.where(lane == h, level, ml)
        acc_out[0, r : r + chunk, columns] = summed
        return jnp.where(lane == h, high, jnp.where(lane == heads + h, total, ml))

    def compute(diagonal):
        for r in range(0, rows, chunk):
            ml = jnp.zeros((chunk, LANES), jnp.float32)
            span = min(r + chunk, keys) if diagonal else keys
            for h in range(heads):
                columns = slice(h * head_size, (h + 1) * head_size)
                q = q_ref[0, r : r + chunk, columns]
                k = kv_ref[:span, columns]
                v = kv_ref[:span, width + h * head_size : width + (h + 1) * head_size]
                bias = (start_ref[slot * heads + h] - gate_ref[h : h + 1, :span]) * LOG2E
                s = lax.dot_general(q, k, (((1,), (1,)), ((), ())), preferred_element_type=jnp.float32)
                s = s + bias
                if diagonal:
                    row = r + lax.broadcasted_iota(jnp.int32, s.shape, 0)
                    s = jnp.where(row >= lax.broadcasted_iota(jnp.int32, s.shape, 1), s, very_low)
                old = state_of(r, h)
                high = jnp.max(s, axis=1, keepdims=True)
                if old is not None:
                    high = jnp.maximum(high, old[0])
                p = jnp.exp2(s - high)
                total = jnp.sum(p, axis=1, keepdims=True)
                summed = jnp.dot(p.astype(jnp.bfloat16), v, preferred_element_type=jnp.float32)
                if old is not None:
                    factor = jnp.exp2(old[0] - high)
                    total = total + factor * old[1]
                    summed = summed + factor * old[2]
                ml = store(r, h, ml, (high, total, summed))
            ml_out[0, r : r + chunk, :] = ml

    if first:
        pl.when(slot == 0)(lambda: compute(True))

        @pl.when((slot > 0) & (mode_ref[slot] > 0))
        def _():
            compute(False)

    else:

        @pl.when(mode_ref[slot] > 0)
        def _():
            compute(False)

    @pl.when((mode_ref[slot] == 0) & ((slot > 0) | (not first)))
    def _():
        for r in range(0, rows, chunk):
            ml = jnp.zeros((chunk, LANES), jnp.float32)
            for h in range(heads):
                old = state_of(r, h)
                if old is None:
                    old = (
                        jnp.full((chunk, 1), very_low, jnp.float32),
                        jnp.zeros((chunk, 1), jnp.float32),
                        jnp.zeros((chunk, head_size), jnp.float32),
                    )
                ml = store(r, h, ml, old)
            ml_out[0, r : r + chunk, :] = ml


def attend_step(mode, starts, queries, pair, gates, state, last, head_size):
    slots, rows, width = queries.shape
    heads = width // head_size
    first = state is None
    chunk = min(rows, 256)
    by_slot = lambda g, *_: (g, 0, 0)
    whole = lambda g, *_: (0, 0)
    in_specs = [
        pl.BlockSpec((1, rows, width), by_slot),
        pl.BlockSpec(pair.shape, whole),
        pl.BlockSpec(gates.shape, whole),
    ]
    state_specs = [pl.BlockSpec((1, rows, width), by_slot), pl.BlockSpec((1, rows, LANES), by_slot)]
    if not first:
        in_specs = in_specs + state_specs
    keys = pair.shape[0]
    return pl.pallas_call(
        functools.partial(attend_kernel, first, last, heads, head_size, chunk),
        out_shape=(
            jax.ShapeDtypeStruct((slots, rows, width), jnp.bfloat16 if last else jnp.float32),
            jax.ShapeDtypeStruct((slots, rows, LANES), jnp.float32),
        ),
        grid_spec=pltpu.PrefetchScalarGridSpec(
            num_scalar_prefetch=2, grid=(slots,), in_specs=in_specs, out_specs=state_specs
        ),
        compiler_params=pltpu.CompilerParams(dimension_semantics=("arbitrary",)),
        cost_estimate=pl.CostEstimate(
            flops=8 * slots * rows * keys * width,
            bytes_accessed=12 * slots * rows * width,
            transcendentals=slots * rows * keys * heads,
        ),
    )(mode, starts, queries, pair, gates, *(() if first else state))


def gathered(block, axis):
    if lax.axis_size(axis) != 2:
        return lax.all_gather(block, axis, axis=1, tiled=True)
    other = swapped(block, axis, 1)
    lower = lax.axis_index(axis) == 0
    return jnp.concatenate([jnp.where(lower, block, other), jnp.where(lower, other, block)], axis=1)


def body(
    tokens,
    input_gain,
    query_weight,
    key_weight,
    value_weight,
    pool_in_weight,
    log_gates,
    pool_weight,
    pool_scale,
    attention_out,
    pooling_out,
    final_gain,
):
    tok_rows = tokens.shape[0]
    width = query_weight.shape[0]
    groups = pool_weight.shape[0]
    head_size = pool_weight.shape[1]
    heads = log_gates.shape[0]
    pool_width = pool_in_weight.shape[1]
    devices = lax.axis_size("sp")
    shards = lax.axis_size("tp")
    side = 1
    while (2 * side) ** 2 <= devices and devices % (2 * side) == 0:
        side = 2 * side
    planes = devices // side
    sequence_index = lax.axis_index("sp")
    plane = sequence_index // side
    seat = sequence_index % side
    first_row = sequence_index * tok_rows

    part = gathered(tokens, "tp")
    gain_part = gathered(input_gain.reshape(1, -1), "tp")
    widened = part.astype(jnp.float32)
    scaled = (widened * gain_part.astype(jnp.float32)).astype(jnp.bfloat16)

    def product(weight):
        return jnp.dot(scaled, weight, preferred_element_type=jnp.float32)

    inverse = lax.rsqrt(jnp.sum(widened * widened, axis=1) / width + epsilon)[:, None]
    keys = (product(key_weight) * inverse).astype(jnp.bfloat16)
    values = (product(value_weight) * inverse).astype(jnp.bfloat16)
    pair = jnp.concatenate([keys, values], axis=1)
    pairs = [pair]
    for _ in range(1, planes):
        pairs.append(passed_along(pairs[-1], "sp", side))
    query = (product(query_weight) * (inverse * (LOG2E * head_size ** (-0.5)))).astype(jnp.bfloat16)
    queries = jnp.stack([query] + [swapped(query, "sp", g) for g in range(1, side)])

    pool_input = (product(pool_in_weight) * inverse).astype(jnp.bfloat16)
    rim = passed_along(pool_input[tok_rows - (WINDOW_MAX - 1) :], "sp", 1)

    seats = seat ^ jnp.arange(side, dtype=jnp.int32)
    starts = jnp.stack(
        [
            lax.dynamic_slice_in_dim(log_gates, (plane * side + (seat ^ g)) * tok_rows, 1, 1)[:, 0]
            for g in range(side)
        ]
    ).reshape(-1)
    state = None
    for k in range(planes):
        source = jnp.maximum(sequence_index - k * side, seat)
        gates = lax.dynamic_slice_in_dim(log_gates, source * tok_rows, tok_rows, 1)
        if k == 0:
            mode = (seats > seat).astype(jnp.int32)
        else:
            mode = jnp.full((side,), plane >= k, jnp.int32)
        state = attend_step(
            mode, starts, queries, pairs[k], gates, state, k == planes - 1, head_size
        )
    partial, level = state
    level = level[:, :, :heads]
    shares = [partial[0]] + [swapped(partial[g], "sp", g) for g in range(1, side)]
    tall = jnp.transpose(level, (0, 2, 1))
    levels = jnp.stack([tall[0]] + [swapped(tall[g], "sp", g) for g in range(1, side)])
    portion = jnp.exp2(levels - jnp.max(levels, axis=0, keepdims=True))
    portion = portion / jnp.sum(portion, axis=0, keepdims=True)
    portion = jnp.transpose(portion, (0, 2, 1))
    attended = 0.0
    for g in range(side):
        attended = attended + shares[g].astype(jnp.float32) * jnp.repeat(portion[g], head_size, axis=1)
    attended = attended.astype(jnp.bfloat16)

    extended = jnp.concatenate([rim, pool_input], axis=0).astype(jnp.float32)
    column = jnp.arange(pool_width, dtype=jnp.int32)
    group_number = lax.axis_index("tp") * groups + column // head_size
    window = jnp.left_shift(jnp.full((pool_width,), 2, jnp.int32), group_number % 4)
    sums = extended
    span = 1
    chosen = jnp.zeros((tok_rows, pool_width), jnp.float32)
    for _ in range(4):
        sums = sums[span:] + sums[:-span]
        span = span * 2
        offset_rows = WINDOW_MAX - span
        chosen = jnp.where(window[None, :] == span, sums[offset_rows : offset_rows + tok_rows], chosen)
    element_locations = first_row + jnp.arange(tok_rows, dtype=jnp.int32)
    counts = jnp.minimum(window[None, :], element_locations[:, None] + 1).astype(jnp.float32)
    departure = (chosen / counts - pool_input.astype(jnp.float32)).astype(jnp.bfloat16)
    mapped = jnp.concatenate(
        [
            jnp.dot(
                departure[:, g * head_size : (g + 1) * head_size],
                pool_weight[g],
                preferred_element_type=jnp.float32,
            )
            for g in range(groups)
        ],
        axis=1,
    )
    pooled = (mapped * pool_scale).astype(jnp.bfloat16)
    pooled_part = jnp.dot(pooled, pooling_out, preferred_element_type=jnp.float32)
    whole = jnp.dot(attended, attention_out, preferred_element_type=jnp.float32) + pooled_part
    if shards == 2:
        half = width // 2
        lower = lax.axis_index("tp") == 0
        sent = jnp.where(lower, whole[:, half:], whole[:, :half]).astype(jnp.bfloat16)
        kept = jnp.where(lower, whole[:, :half], whole[:, half:])
        mixed = kept + swapped(sent, "tp", 1).astype(jnp.float32)
        squares = jnp.sum(mixed * mixed, axis=1)
        squares = squares + swapped(squares, "tp", 1)
    else:
        mixed = lax.psum_scatter(
            whole.astype(jnp.bfloat16), "tp", scatter_dimension=1, tiled=True
        ).astype(jnp.float32)
        squares = lax.psum(jnp.sum(mixed * mixed, axis=1), "tp")
    out_inverse = lax.rsqrt(squares / width + epsilon)
    return (mixed * out_inverse[:, None] * final_gain[None, :]).astype(jnp.bfloat16)


def solution(mesh):
    return jax.shard_map(
        body,
        mesh=mesh,
        in_specs=(
            P("sp", "tp"),
            P("tp"),
            P(None, "tp"),
            P(None, "tp"),
            P(None, "tp"),
            P(None, "tp"),
            P("tp", None),
            P("tp", None, None),
            P("tp"),
            P("tp", None),
            P("tp", None),
            P("tp"),
        ),
        out_specs=P("sp", "tp"),
        check_vma=False,
    )
```
